768 devices in a mesh: row: 48 (over z, x), col: 16 (over y, core).
Axes of the slice: x: 4, y: 8, z: 12, core: 2. Of those that a mesh axis runs over, the one named last changes fastest.
Arguments:
- tokens: bfloat16 [55296, 4096], P('row'), may hold values from -6 to 6
- proj_in: bfloat16 [4096, 2048], P(None, 'col'), may hold values from -0.09375 to 0.09375
- proj_out: bfloat16 [2048, 4096], P(None, 'col'), may hold values from -0.125 to 0.125
Outputs:
- mixed: bfloat16 [55296, 4096], P('row', 'col')
The draws below stay inside these ranges and needn't reach their ends.
All inputs are finite; a program needn't handle non-finite values.
Results may differ from the reference program's by a relative error of at most 0.0057.
Values may be sent and summed in bfloat16 or wider, within the bound.
A program may use at most 64 MiB of HBM per device.

```python
import jax
import jax.numpy as jnp

D = 4096
GW = 128
SEQ = 55296
FW = 2048
N_COL = 16


def levels(key, dims, cuts, low, high):
    factor_of, own = 1.0, jax.random.fold_in(key, 6)
    for position, parts in cuts:
        steps = jnp.exp(jax.random.uniform(jax.random.fold_in(own, position), (parts,), jnp.float32, low / len(cuts), high / len(cuts)))
        factor_of = factor_of * jnp.repeat(steps, dims[position] // parts).reshape([-1 if axis == position else 1 for axis in range(len(dims))])
    return factor_of


def centred(rng, dims, width, limit, pieces=(), kind=jnp.bfloat16):
    gain = levels(rng, dims, pieces, -0.22, 0.18) if pieces else 1.0
    result = jax.random.normal(rng, dims, jnp.float32) * width * gain
    return jnp.minimum(jnp.maximum(result, -limit), limit).astype(kind)


def setup_inputs(seed: int = 0) -> dict:
    key_of = jax.random.split(jax.random.key(seed), 4)
    tokens = centred(key_of[0], (SEQ, D), 1.0, 6.0, ((0, 48),))
    proj_in = centred(key_of[1], (D, FW), D ** -0.5, 0.09375, ((1, 16),))
    proj_out = centred(key_of[2], (FW, D), FW ** -0.5, 0.125, ((1, 16),))
    return dict(tokens=tokens, proj_in=proj_in, proj_out=proj_out)


def reference(tokens, proj_in, proj_out):
    branch_in = jnp.dot(tokens, proj_in, preferred_element_type=jnp.float32).astype(jnp.bfloat16)
    grouped = branch_in.astype(jnp.float32).reshape(SEQ, N_COL, GW)
    spectrum = jnp.fft.fft2(grouped, axes=(0, 2), norm="ortho").real
    spectrum = spectrum.astype(jnp.bfloat16).reshape(SEQ, FW)
    return jnp.dot(spectrum, proj_out, preferred_element_type=jnp.float32).astype(jnp.bfloat16)
```

```python
import functools
import math

import jax
import jax.numpy as jnp
import numpy as np
from jax import lax
from jax.experimental import pallas as pl
from jax.experimental.pallas import tpu as pltpu
from jax.sharding import PartitionSpec as P

MESH = pl.DeviceIdType.MESH
BF16 = jnp.bfloat16
F32 = jnp.float32


def exchange_kernel(n, src, dst, send_sem, recv_sem):
    me = lax.axis_index("row")
    barrier = pltpu.get_barrier_semaphore()

    def greet(s, carry):
        peer = lax.rem(me + s, n)
        pl.semaphore_signal(barrier, inc=1, device_id={"row": peer}, device_id_type=MESH)
        return carry

    lax.fori_loop(1, n, greet, 0)
    pl.semaphore_wait(barrier, n - 1)

    def send(s, carry):
        peer = lax.rem(me + s, n)
        pltpu.make_async_remote_copy(
            src_ref=src.at[peer],
            dst_ref=dst.at[me],
            send_sem=send_sem,
            recv_sem=recv_sem,
            device_id={"row": peer},
            device_id_type=MESH,
        ).start()
        return carry

    lax.fori_loop(1, n, send, 0)
    dst[me] = src[me]
    rest = dst.at[pl.ds(0, n - 1)]
    pltpu.make_async_copy(rest, rest, recv_sem).wait()
    pltpu.make_async_copy(rest, rest, send_sem).wait()


def exchange(blocks, ident):
    n = blocks.shape[0]
    return pl.pallas_call(
        functools.partial(exchange_kernel, n),
        out_shape=jax.ShapeDtypeStruct(blocks.shape, blocks.dtype),
        in_specs=[pl.BlockSpec(memory_space=pltpu.VMEM)],
        out_specs=pl.BlockSpec(memory_space=pltpu.VMEM),
        scratch_shapes=[pltpu.SemaphoreType.DMA, pltpu.SemaphoreType.DMA],
        compiler_params=pltpu.CompilerParams(collective_id=ident, has_side_effects=True),
    )(blocks)


def cos_sin(phase, period):
    angles = phase.astype(F32) * (2.0 * math.pi / period)
    return jnp.cos(angles), jnp.sin(angles)


def channel_table(width):
    half = width // 2
    j = np.arange(width)
    l = np.arange(half)
    table = np.zeros((width, width))
    table[:, :half] = np.cos(2 * np.pi * np.outer(j, l) / width)
    table[:, half:] = -np.sin(2 * np.pi * np.outer(j, l) / width)
    table[:, half] = (-1.0) ** j
    return table


def on_device(tokens, proj_in, proj_out):
    n = lax.axis_size("row")
    rank = lax.axis_index("row")
    rows = tokens.shape[0]
    width = proj_in.shape[1]
    half = width // 2
    total = rows * n
    inner = rows // n
    branch_in = jnp.dot(tokens, proj_in, preferred_element_type=F32).astype(BF16)
    chan = jnp.asarray(channel_table(width), BF16)
    mixed = jnp.dot(branch_in, chan, preferred_element_type=F32).astype(BF16)
    blocks = mixed.reshape(inner, n, width).transpose(1, 0, 2)
    data = exchange(blocks, 0).reshape(rows, width)
    d = np.arange(n)[:, None]
    a = np.arange(inner)[None, :]
    freq = np.where(a < inner // 2, 48 * a + d, n * a + (n - d) % n).reshape(-1)
    times = n * jnp.arange(rows, dtype=jnp.int32) + rank
    phase = (jnp.asarray(freq, jnp.int32)[:, None] * times[None, :]) % total
    tc, ts = cos_sin(phase, total)
    g = jnp.dot(tc.astype(BF16), data, preferred_element_type=F32)
    h = jnp.dot(ts.astype(BF16), data, preferred_element_type=F32)
    g = g + jnp.concatenate([h[:, half:], -h[:, :half]], axis=1)
    parts = exchange(g.astype(BF16).reshape(n, inner, width), 1)
    mirror = jnp.where(rank == 0, (inner - np.arange(inner)) % inner, inner - 1 - np.arange(inner))
    other = jnp.take(parts, mirror, axis=1)
    b = np.arange(n)
    p = np.arange(n)

    def tab(rows_):
        ang = 2 * np.pi * (np.outer(rows_, p) % n) / n
        return np.concatenate([np.cos(ang), np.sin(ang)], axis=1)

    fwd = jnp.asarray(tab(b), BF16)
    rev = jnp.asarray(tab(n - 1 - b), BF16)
    rev0 = jnp.asarray(tab((n - b) % n), BF16)
    er, ei = parts[:, :, :half], parts[:, :, half:]
    fr, fi = other[:, :, :half], other[:, :, half:]
    first = (np.arange(half) == 0)[None, None, :]
    zero = jnp.zeros_like(er)
    half_ = jnp.asarray(0.5, BF16)
    x1 = jnp.concatenate([jnp.where(first, er * half_, er), jnp.where(first, ei * half_, zero)], axis=2)
    x2 = jnp.concatenate([jnp.where(first, ei * half_, ei), jnp.where(first, -er * half_, zero)], axis=2)
    x3 = jnp.concatenate([jnp.where(first, fr * half_, zero), jnp.where(first, fi * half_, fr)], axis=2)
    x4 = jnp.concatenate([jnp.where(first, fi * half_, zero), jnp.where(first, -fr * half_, fi)], axis=2)
    xa = jnp.concatenate([x1, x2], axis=0)
    xb = jnp.concatenate([x3, x4], axis=0)
    out = jnp.einsum("bp,pal->bal", fwd, xa, preferred_element_type=F32)
    out_m = jnp.einsum("bp,pal->bal", rev, xb, preferred_element_type=F32)
    out_0 = jnp.einsum("bp,pl->bl", rev0, xb[:, 0], preferred_element_type=F32)
    out_m = jnp.concatenate([jnp.where(rank == 0, out_0, out_m[:, 0])[:, None], out_m[:, 1:]], axis=1)
    spec = ((out + out_m) * (1.0 / math.sqrt(total * width))).astype(BF16)
    last = exchange(spec, 2)
    low = last[:, : inner // 2].transpose(1, 0, 2)
    up = last[:, inner // 2 :]
    up = jnp.concatenate([up[:1], up[1:][::-1]], axis=0).transpose(1, 0, 2)
    spectrum = jnp.concatenate([low, up], axis=0).reshape(rows, width)
    perm = np.concatenate([np.arange(half), [half], width - np.arange(1, half)])
    weights = proj_out.reshape(-1, width, proj_out.shape[1])[:, perm].reshape(proj_out.shape)
    gathered = lax.all_gather(spectrum, "col", axis=1, tiled=True)
    return jnp.dot(gathered, weights, preferred_element_type=F32).astype(BF16)


def solution(mesh):
    return jax.shard_map(
        on_device,
        mesh=mesh,
        in_specs=(P("row", None), P(None, "col"), P(None, "col")),
        out_specs=P("row", "col"),
        check_vma=False,
    )
```

```python
import functools
import math

import jax
import jax.numpy as jnp
from jax import lax
from jax.experimental import pallas as pl
from jax.experimental.pallas import tpu as pltpu
from jax.sharding import PartitionSpec as P

MESH = pl.DeviceIdType.MESH
BF16 = jnp.bfloat16
F32 = jnp.float32
CHUNKS = 3


def turn(phase, period):
    wraps = jnp.floor(phase * (1.0 / period) + 0.5)
    x = (phase - wraps * period) * (math.pi / period)
    y = x * x
    s = 1.0 + y * (-1 / 6 + y * (1 / 120 + y * (-1 / 5040 + y * (1 / 362880 + y * (-1 / 39916800)))))
    c = 1.0 + y * (
        -1 / 2 + y * (1 / 24 + y * (-1 / 720 + y * (1 / 40320 + y * (-1 / 3628800 + y * (1 / 479001600)))))
    )
    s = s * x
    return 1.0 - 2.0 * s * s, 2.0 * s * c


def iota(shape, axis):
    return lax.broadcasted_iota(jnp.int32, shape, axis)


def dot(a, b):
    return jnp.dot(a, b, preferred_element_type=F32)


def kernel(
    n,
    ncol,
    tokens,
    proj_in,
    proj_out,
    out,
    tok,
    win,
    wout,
    table,
    base_c,
    base_s,
    work,
    gacc,
    send1,
    recv1,
    send2,
    recv2,
    send3,
    recv3,
    gath,
    upper,
    load_sem,
    xs,
    xr,
    rs_sem,
    rr_sem,
    ls_sem,
    lr_sem,
    ss_sem,
    sr_sem,
):
    rank = lax.axis_index("row")
    col = lax.axis_index("col")
    core = lax.rem(col, 2)
    right = lax.rem(col + 2, ncol)
    left = lax.rem(col + ncol - 2, ncol)
    sib = col + 1 - 2 * core
    rows, depth = tokens.shape
    width = proj_in.shape[1]
    half = width // 2
    total = rows * n
    part = rows // CHUNKS
    per = part // n

    barrier = pltpu.get_barrier_semaphore()

    def greet(s, carry):
        pl.semaphore_signal(
            barrier, inc=1, device_id={"row": lax.rem(rank + s, n)}, device_id_type=MESH
        )
        return carry

    lax.fori_loop(1, n, greet, 0)
    for peer in (right, left, sib):
        pl.semaphore_signal(barrier, inc=1, device_id={"col": peer}, device_id_type=MESH)

    load_in = pltpu.make_async_copy(proj_in, win, load_sem.at[CHUNKS])
    load_in.start()
    loads = []
    for c in range(CHUNKS):
        block = pl.ds(c * part, part)
        load = pltpu.make_async_copy(tokens.at[block], tok.at[block], load_sem.at[c])
        load.start()
        loads.append(load)
    load_out = pltpu.make_async_copy(proj_out, wout, load_sem.at[CHUNKS + 1])
    load_out.start()

    def post(src, dst, which):
        def send(s, carry):
            peer = lax.rem(rank + s, n)
            pltpu.make_async_remote_copy(
                src_ref=src.at[peer],
                dst_ref=dst.at[rank],
                send_sem=xs.at[which],
                recv_sem=xr.at[which],
                device_id={"row": peer},
                device_id_type=MESH,
            ).start()
            return carry

        lax.fori_loop(1, n, send, 0)
        dst[rank] = src[rank]

    def arrived(dst, which):
        rest = dst.at[pl.ds(0, n - 1)]
        pltpu.make_async_copy(rest, rest, xr.at[which]).wait()

    def flat(ref):
        return ref[...].astype(F32).reshape(part, width)

    def blocks(value):
        return value.reshape(n, per, width).astype(BF16)

    lane = iota((width, width), 1)
    j = iota((width, width), 0)
    l = jnp.where(lane < half, lane, jnp.where(lane == half, half, lane - half))
    cc, sc = turn((j * l).astype(F32), width)
    chan = jnp.where(lane <= half, cc, -sc).astype(BF16)

    load_in.wait()
    for c in range(CHUNKS):
        loads[c].wait()
        x = dot(tok[pl.ds(c * part, part), :], win[...]).astype(BF16)
        work[...] = dot(x, chan)
        for p in range(n):
            send1[c, p] = work[pl.ds(p, per, stride=n), :].astype(BF16)
        if c == 0:
            pl.semaphore_wait(barrier, n - 1 + 3)
        post(send1.at[c], recv1.at[c], c)

    lanes = rows
    li = iota((8, lanes), 1)
    cq = jnp.where(li >= 2 * part, 2, jnp.where(li >= part, 1, 0))
    rem = li - cq * part
    t = n // 2 * (rem // per) + per * cq + rem % per
    time = (n * t + rank).astype(F32)
    ri = iota((8, lanes), 0)
    for g in range(n // 8):
        bc, bs = turn((ri + 8 * g).astype(F32) * time, total)
        base_c[pl.ds(8 * g, 8), :] = bc
        base_s[pl.ds(8 * g, 8), :] = bs
    sigma = jnp.where(ri < 4, 1.0, -1.0).astype(F32)

    def fill(ca, pair, wc, ws, wcs, wss):
        cos, sin = [], []
        for k in range(2):
            bc = base_c[pl.ds(2 * pair + k, 1), :]
            bs = base_s[pl.ds(2 * pair + k, 1), :]
            cos.append(wc * bc - wss * bs)
            sin.append(ws * bc + wcs * bs)
        at = pl.multiple_of(16 * pair, 16)
        table[ca, pl.ds(at, 16), :] = jnp.concatenate(cos, axis=0).astype(BF16)
        table[ca, pl.ds(part + at, 16), :] = jnp.concatenate(sin, axis=0).astype(BF16)

    for ca in range(CHUNKS):
        num = jnp.where(ri < 4, 4 * ca + ri, 17 - 4 * ca + ri)
        wc, ws = turn(num.astype(F32) * time, rows)

        def body(pair, carry, ca=ca, wc=wc, ws=ws):
            fill(ca, pair, wc, ws, wc * sigma, ws * sigma)
            return carry

        lax.fori_loop(0, n // 2, body, 0)
        if ca == 0:
            ac, as_ = turn(jnp.float32(12.0) * time, rows)
            bc1 = base_c[pl.ds(1, 1), :]
            bs1 = base_s[pl.ds(1, 1), :]
            mid = ri == 7
            cos0 = jnp.where(mid, ac, wc)
            sin0 = jnp.where(mid, as_, ws)
            cos1 = wc * bc1 - ws * sigma * bs1
            sin1 = ws * bc1 + wc * sigma * bs1
            table[0, pl.ds(0, 16), :] = jnp.concatenate([cos0, cos1], axis=0).astype(BF16)
            table[0, pl.ds(part, 16), :] = jnp.concatenate([sin0, sin1], axis=0).astype(BF16)

    bi = iota((n, 4 * n), 0)
    pi = iota((n, 4 * n), 1)
    quarter = jnp.where(pi >= 3 * n, 3, jnp.where(pi >= 2 * n, 2, jnp.where(pi >= n, 1, 0)))
    pp = pi - quarter * n

    def outer(flip):
        bb = jnp.where(quarter < 2, bi, flip - bi)
        oc, os = turn((bb * pp).astype(F32), n)
        return jnp.where((quarter == 0) | (quarter == 2), oc, os)

    at_zero = rank == 0
    tab = outer(n - 1)
    tab_zero = jnp.where(at_zero, outer(n), tab).astype(BF16)
    tab = tab.astype(BF16)

    qr = iota((width, width), 0)
    qc = iota((width, width), 1)
    chosen = jnp.where(qr <= half, qr, width + half - qr)
    swap = jnp.where(qc == chosen, 1.0, 0.0).astype(BF16)
    load_out.wait()

    def reorder(g, carry):
        at = pl.ds(pl.multiple_of(g * width, width), width)
        wout[at, :] = dot(swap, wout[at, :]).astype(BF16)
        return carry

    lax.fori_loop(0, ncol, reorder, 0)

    pr = iota((part, part), 0)
    pc = iota((part, part), 1)
    want_i = pr // n
    want_e = pr - want_i * n
    want_d = jnp.where(want_i < 4, want_e, jnp.where(want_e == 0, 0, n - want_e))
    order = jnp.where(pc == want_d * per + want_i, 1.0, 0.0).astype(BF16)

    sign = jnp.where(iota((part, width), 1) < half, 1.0, -1.0).astype(F32)
    for c in range(CHUNKS):
        arrived(recv1.at[c], c)
        data = flat(recv1.at[c]).astype(BF16)
        for ca in range(CHUNKS):
            got = dot(table[ca, :, pl.ds(c * part, part)], data)
            if c > 0:
                got = gacc[ca] + got
            if c < CHUNKS - 1:
                gacc[ca] = got
            else:
                value = got[:part] + pltpu.roll(got[part:], half, 1) * sign
                send2[ca] = blocks(value)
                if ca < 2:
                    post(send2.at[ca], recv2.at[ca], 3 + ca)

    lane48 = iota((n, width), 1)
    m1 = jnp.where((lane48 == 0) | (lane48 == half), 0.5, jnp.where(lane48 < half, 1.0, 0.0)).astype(F32)
    m2 = jnp.where(lane48 == half, -0.5, m1).astype(F32)
    m3 = jnp.where((lane48 == 0) | (lane48 == half), 0.5, 0.0).astype(F32)
    m4 = jnp.where(lane48 > half, 1.0, 0.0).astype(F32)
    m5 = jnp.where(lane48 == half, -0.5, m3).astype(F32)
    scale = 1.0 / math.sqrt(total * width)

    def outer_stage(ca):
        arrived(recv2.at[ca], 3 + ca)
        work[...] = flat(recv2.at[ca])
        parts = [work[pl.ds(i, n, stride=per), :] for i in range(per)]
        for i in range(per):
            ea, eb, lhs = parts[i], parts[per - 1 - i], tab
            if ca == 0 and i in (0, per - 1):
                eb = jnp.where(at_zero, ea, eb)
            if ca == 0 and i == 0:
                lhs = tab_zero
            ra = pltpu.roll(ea, half, 1)
            rb = pltpu.roll(eb, half, 1)
            z = jnp.concatenate(
                [
                    (ea * m1).astype(BF16),
                    (ra * m2).astype(BF16),
                    (eb * m3 + rb * m4).astype(BF16),
                    (eb * m4 + rb * m5).astype(BF16),
                ],
                axis=0,
            )
            work[pl.ds(i, n, stride=per), :] = dot(lhs, z) * scale
        send3[ca] = blocks(work[...])
        post(send3.at[ca], recv3.at[ca], 6 + ca)

    piece_rows = part // 2
    pending = []

    def ring(ca, slot, h, peer, s_sem, r_sem):
        at = gath.at[ca].at[slot].at[pl.ds(h * piece_rows, piece_rows)]
        return pltpu.make_async_remote_copy(
            src_ref=at,
            dst_ref=at,
            send_sem=s_sem,
            recv_sem=r_sem,
            device_id={"col": peer},
            device_id_type=MESH,
        )

    def go(*args):
        copy = ring(*args)
        copy.start()
        pending.append(copy)

    def gather_start(ca):
        arrived(recv3.at[ca], 6 + ca)
        gath[ca, col] = dot(order, flat(recv3.at[ca]).astype(BF16)).astype(BF16)
        go(ca, col, 0, right, rs_sem.at[ca, 0], rr_sem.at[ca, 0])
        go(ca, col, 1, left, ls_sem.at[ca, 0], lr_sem.at[ca, 0])
        go(ca, col, 1, right, rs_sem.at[ca, 1], rr_sem.at[ca, 1])
        go(ca, col, 0, left, ls_sem.at[ca, 1], lr_sem.at[ca, 1])
        go(ca, col, 0, sib, ss_sem.at[ca, 0], sr_sem.at[ca, 0])
        go(ca, col, 1, sib, ss_sem.at[ca, 1], sr_sem.at[ca, 1])

    steps = ncol // 2 - 1

    def gather_step(ca, i):
        dist = i // 2 + 1
        slot = lax.rem(col + ncol - 2 * dist, ncol)
        h = i % 2
        ring(ca, slot, h, right, rs_sem.at[ca, i], rr_sem.at[ca, i]).wait_recv()
        if i + 2 < steps:
            go(ca, slot, h, right, rs_sem.at[ca, i + 2], rr_sem.at[ca, i + 2])
        go(ca, slot, h, sib, ss_sem.at[ca, 2 + 2 * i], sr_sem.at[ca, 2 + 2 * i])
        slot = lax.rem(col + 2 * dist, ncol)
        h = 1 - i % 2
        ring(ca, slot, h, left, ls_sem.at[ca, i], lr_sem.at[ca, i]).wait_recv()
        if i + 2 < steps:
            go(ca, slot, h, left, ls_sem.at[ca, i + 2], lr_sem.at[ca, i + 2])
        go(ca, slot, h, sib, ss_sem.at[ca, 3 + 2 * i], sr_sem.at[ca, 3 + 2 * i])

    def project(ca):
        for i in range(2 * steps + 2):
            ring(ca, 0, 0, sib, ss_sem.at[ca, i], sr_sem.at[ca, i]).wait_recv()
        acc = None
        for y in range(ncol // 2):
            lhs = jnp.concatenate([gath[ca, 2 * y], gath[ca, 2 * y + 1]], axis=1)
            term = dot(lhs, wout[pl.ds(2 * width * y, 2 * width), :])
            acc = term if acc is None else acc + term
        low = part // 2
        out[pl.ds(low * ca, low), :] = acc[:low].astype(BF16)
        upper[pl.ds(low * (CHUNKS - 1 - ca), low), :] = acc[low:]

    def steps_of(ca, first, last):
        for i in range(first, last):
            gather_step(ca, i)

    outer_stage(0)
    post(send2.at[2], recv2.at[2], 5)
    outer_stage(1)
    gather_start(0)
    steps_of(0, 0, 3)
    outer_stage(2)
    steps_of(0, 3, steps)
    gather_start(1)
    project(0)
    steps_of(1, 0, 4)
    gather_start(2)
    steps_of(1, 4, steps)
    project(1)
    steps_of(2, 0, steps)
    project(2)
    edge = [upper[pl.ds(n * k, 1), :] for k in range(n // 4)]
    for k in range(n // 4):
        upper[pl.ds(n * ((k + 1) % (n // 4)), 1), :] = edge[k]
    out[pl.ds(rows // 2, rows // 2), :] = upper[...].astype(BF16)
    for copy in pending:
        copy.wait_send()
    for which in range(3 * CHUNKS):
        rest = recv1.at[0].at[pl.ds(0, n - 1)]
        pltpu.make_async_copy(rest, rest, xs.at[which]).wait()


def on_device(tokens, proj_in, proj_out):
    n = lax.axis_size("row")
    ncol = lax.axis_size("col")
    rows, depth = tokens.shape
    width = proj_in.shape[1]
    part = rows // CHUNKS
    steps = ncol // 2 - 1
    anywhere = pl.BlockSpec(memory_space=pl.ANY)
    message = pltpu.VMEM((CHUNKS, n, part // n, width), BF16)
    dma = pltpu.SemaphoreType.DMA
    return pl.pallas_call(
        functools.partial(kernel, n, ncol),
        out_shape=jax.ShapeDtypeStruct((rows, proj_out.shape[1]), BF16),
        in_specs=[anywhere] * 3,
        out_specs=pl.BlockSpec(memory_space=pltpu.VMEM),
        scratch_shapes=[
            pltpu.VMEM(tokens.shape, BF16),
            pltpu.VMEM(proj_in.shape, BF16),
            pltpu.VMEM(proj_out.shape, BF16),
            pltpu.VMEM((CHUNKS, 2 * part, rows), BF16),
            pltpu.VMEM((n, rows), F32),
            pltpu.VMEM((n, rows), F32),
            pltpu.VMEM((part, width), F32),
            pltpu.VMEM((CHUNKS, 2 * part, width), F32),
            message,
            message,
            message,
            message,
            message,
            message,
            pltpu.VMEM((CHUNKS, ncol, part, width), BF16),
            pltpu.VMEM((rows // 2, proj_out.shape[1]), F32),
            dma((CHUNKS + 2,)),
            dma((3 * CHUNKS,)),
            dma((3 * CHUNKS,)),
            dma((CHUNKS, steps)),
            dma((CHUNKS, steps)),
            dma((CHUNKS, steps)),
            dma((CHUNKS, steps)),
            dma((CHUNKS, 2 * steps + 2)),
            dma((CHUNKS, 2 * steps + 2)),
        ],
        compiler_params=pltpu.CompilerParams(
            collective_id=0, has_side_effects=True, vmem_limit_bytes=60 * 1024 * 1024
        ),
    )(tokens, proj_in, proj_out)


def solution(mesh):
    return jax.shard_map(
        on_device,
        mesh=mesh,
        in_specs=(P("row", None), P(None, "col"), P(None, "col")),
        out_specs=P("row", "col"),
        check_vma=False,
    )
```

```python
import functools
import math

import jax
import jax.numpy as jnp
from jax import lax
from jax.experimental import pallas as pl
from jax.experimental.pallas import tpu as pltpu
from jax.sharding import PartitionSpec as P

MESH = pl.DeviceIdType.MESH
BF16 = jnp.bfloat16
F32 = jnp.float32
CHUNKS = 3
SIZES = (8, 8, 8)


def turn(phase, period):
    wraps = jnp.floor(phase * (1.0 / period) + 0.5)
    x = (phase - wraps * period) * (math.pi / period)
    y = x * x
    s = 1.0 + y * (-1 / 6 + y * (1 / 120 + y * (-1 / 5040 + y * (1 / 362880 + y * (-1 / 39916800)))))
    c = 1.0 + y * (
        -1 / 2 + y * (1 / 24 + y * (-1 / 720 + y * (1 / 40320 + y * (-1 / 3628800 + y * (1 / 479001600)))))
    )
    s = s * x
    return 1.0 - 2.0 * s * s, 2.0 * s * c


def iota(shape, axis):
    return lax.broadcasted_iota(jnp.int32, shape, axis)


def dot(a, b):
    return jnp.dot(a, b, preferred_element_type=F32)


def kernel(
    n,
    ncol,
    tokens,
    proj_in,
    proj_out,
    out,
    tok,
    win,
    wout,
    table,
    base_c,
    base_s,
    work,
    gacc,
    send1,
    recv1,
    upper,
    load_sem,
    xs,
    xr,
    rr_sem,
    lr_sem,
    ss_sem,
    sr_sem,
    *rest,
):
    parts_ = len(SIZES)
    send2, recv2, send3, recv3, gath = (rest[k * parts_ : (k + 1) * parts_] for k in range(5))
    starts = [sum(SIZES[:c]) for c in range(parts_)]
    rank = lax.axis_index("row")
    col = lax.axis_index("col")
    core = lax.rem(col, 2)
    right = lax.rem(col + 2, ncol)
    left = lax.rem(col + ncol - 2, ncol)
    sib = col + 1 - 2 * core
    rows, depth = tokens.shape
    width = proj_in.shape[1]
    half = width // 2
    total = rows * n
    part = rows // CHUNKS
    per = part // n

    barrier = pltpu.get_barrier_semaphore()

    def greet(s, carry):
        pl.semaphore_signal(
            barrier, inc=1, device_id={"row": lax.rem(rank + s, n)}, device_id_type=MESH
        )
        return carry

    lax.fori_loop(1, n, greet, 0)
    for peer in (right, left, sib):
        pl.semaphore_signal(barrier, inc=1, device_id={"col": peer}, device_id_type=MESH)

    load_in = pltpu.make_async_copy(proj_in, win, load_sem.at[CHUNKS])
    load_in.start()
    loads = []
    for c in range(CHUNKS):
        block = pl.ds(c * part, part)
        load = pltpu.make_async_copy(tokens.at[block], tok.at[block], load_sem.at[c])
        load.start()
        loads.append(load)
    load_out = pltpu.make_async_copy(proj_out, wout, load_sem.at[CHUNKS + 1])
    load_out.start()

    def post(src, dst, which):
        def send(peer):
            pltpu.make_async_remote_copy(
                src_ref=src.at[peer],
                dst_ref=dst.at[rank],
                send_sem=xs.at[which],
                recv_sem=xr.at[which],
                device_id={"row": peer},
                device_id_type=MESH,
            ).start()

        def both(s, carry):
            up = rank + (n // 2 - s)
            down = rank - (n // 2 - s)
            send(jnp.where(up >= n, up - n, up))
            send(jnp.where(down < 0, down + n, down))
            return carry

        opposite = rank + n // 2
        send(jnp.where(opposite >= n, opposite - n, opposite))
        lax.fori_loop(1, n // 2, both, 0)
        dst[rank] = src[rank]

    def post2(k):
        post(send2[k], recv2[k], CHUNKS + k)

    def arrived(dst, which):
        rest = dst.at[pl.ds(0, n - 1)]
        pltpu.make_async_copy(rest, rest, xr.at[which]).wait()

    def flat(ref):
        return ref[...].astype(F32).reshape(n * ref.shape[1], width)

    def blocks(value):
        return value.reshape(n, value.shape[0] // n, width).astype(BF16)

    lane = iota((width, width), 1)
    j = iota((width, width), 0)
    l = jnp.where(lane < half, lane, jnp.where(lane == half, half, lane - half))
    cc, sc = turn((j * l).astype(F32), width)
    chan = jnp.where(lane <= half, cc, -sc).astype(BF16)

    load_in.wait()
    for c in range(CHUNKS):
        with jax.named_scope(f"tokens{c}"):
            loads[c].wait()
        with jax.named_scope(f"branch{c}"):
            x = dot(tok[pl.ds(c * part, part), :], win[...]).astype(BF16)
            work[...] = dot(x, chan)
            for p in range(n):
                send1[c, p] = work[pl.ds(p, per, stride=n), :].astype(BF16)
        if c == 0:
            with jax.named_scope("barrier"):
                pl.semaphore_wait(barrier, n - 1 + 3)
        with jax.named_scope(f"post1_{c}"):
            post(send1.at[c], recv1.at[c], c)

    with jax.named_scope("tables"):
        lanes = rows
        li = iota((8, lanes), 1)
        cq = jnp.where(li >= 2 * part, 2, jnp.where(li >= part, 1, 0))
        rem = li - cq * part
        t = n // 2 * (rem // per) + per * cq + rem % per
        time = (n * t + rank).astype(F32)
        ri = iota((8, lanes), 0)
        for g in range(n // 8):
            bc, bs = turn((ri + 8 * g).astype(F32) * time, total)
            base_c[pl.ds(8 * g, 8), :] = bc
            base_s[pl.ds(8 * g, 8), :] = bs

        for c, size in enumerate(SIZES):
            start = starts[c] // 2
            place = ri % size
            lower = place < size // 2
            num = jnp.where(lower, start + place, 25 - start - size + place)
            sigma = jnp.where(lower, 1.0, -1.0).astype(F32)
            wc, ws = turn(num.astype(F32) * time, rows)
            wcs, wss = wc * sigma, ws * sigma
            each = 8 // size
            row = 2 * n * starts[c]

            def unit(u, wc=wc, ws=ws, wcs=wcs, wss=wss, each=each):
                bc = base_c[pl.ds(u * each, 1), :]
                bs = base_s[pl.ds(u * each, 1), :]
                if each == 2:
                    bc = jnp.where(ri < 4, bc, base_c[pl.ds(2 * u + 1, 1), :])
                    bs = jnp.where(ri < 4, bs, base_s[pl.ds(2 * u + 1, 1), :])
                return wc * bc - wss * bs, ws * bc + wcs * bs

            def put(pair, first, second, row=row, size=size):
                at = pl.multiple_of(row + 16 * pair, 16)
                table[pl.ds(at, 16), :] = jnp.concatenate([first[0], second[0]], axis=0).astype(BF16)
                at = pl.multiple_of(row + n * size + 16 * pair, 16)
                table[pl.ds(at, 16), :] = jnp.concatenate([first[1], second[1]], axis=0).astype(BF16)

            def body(pair, carry, unit=unit, put=put):
                put(pair, unit(2 * pair), unit(2 * pair + 1))
                return carry

            lax.fori_loop(0, n * size // 16, body, 0)
            if c == 0:
                mc, ms = turn(jnp.float32(12.0) * time, rows)
                oc, os = unit(0)
                mid = ri == size - 1
                put(0, (jnp.where(mid, mc, oc), jnp.where(mid, ms, os)), unit(1))

    with jax.named_scope("tables2"):
        bi = iota((n, 4 * n), 0)
        pi = iota((n, 4 * n), 1)
        quarter = jnp.where(pi >= 3 * n, 3, jnp.where(pi >= 2 * n, 2, jnp.where(pi >= n, 1, 0)))
        pp = pi - quarter * n

        def outer(flip):
            bb = jnp.where(quarter < 2, bi, flip - bi)
            oc, os = turn((bb * pp).astype(F32), n)
            return jnp.where((quarter == 0) | (quarter == 2), oc, os)

        at_zero = rank == 0
        tab = outer(n - 1)
        tab_zero = jnp.where(at_zero, outer(n), tab).astype(BF16)
        tab = tab.astype(BF16)

        qr = iota((width, width), 0)
        qc = iota((width, width), 1)
        chosen = jnp.where(qr <= half, qr, width + half - qr)
        swap = jnp.where(qc == chosen, 1.0, 0.0).astype(BF16)
        load_out.wait()

        def reorder(g, carry):
            at = pl.ds(pl.multiple_of(g * width, width), width)
            wout[at, :] = dot(swap, wout[at, :]).astype(BF16)
            return carry

        lax.fori_loop(0, ncol, reorder, 0)

        orders = {}
        for size in sorted(set(SIZES)):
            pr = iota((n * size, n * size), 0)
            pc = iota((n * size, n * size), 1)
            want_i = pr // n
            want_e = pr - want_i * n
            want_d = jnp.where(want_i < size // 2, want_e, jnp.where(want_e == 0, 0, n - want_e))
            orders[size] = jnp.where(pc == want_d * size + want_i, 1.0, 0.0).astype(BF16)

    sign = jnp.where(iota((part, width), 1) < half, 1.0, -1.0).astype(F32)
    for c in range(CHUNKS):
        with jax.named_scope(f"wait1_{c}"):
            arrived(recv1.at[c], c)
        data = flat(recv1.at[c]).astype(BF16)
        for k, size in enumerate(SIZES):
            at = pl.ds(2 * n * starts[k], 2 * n * size)
            got = dot(table[at, pl.ds(c * part, part)], data)
            if c > 0:
                got = gacc[at, :] + got
            if c < CHUNKS - 1:
                gacc[at, :] = got
            else:
                value = got[: n * size] + pltpu.roll(got[n * size :], half, 1) * sign[: n * size]
                send2[k][...] = blocks(value)
                if k < 2:
                    with jax.named_scope(f"post2_{k}"):
                        post2(k)

    lane48 = iota((n, width), 1)
    m1 = jnp.where((lane48 == 0) | (lane48 == half), 0.5, jnp.where(lane48 < half, 1.0, 0.0)).astype(F32)
    m2 = jnp.where(lane48 == half, -0.5, m1).astype(F32)
    m3 = jnp.where((lane48 == 0) | (lane48 == half), 0.5, 0.0).astype(F32)
    m4 = jnp.where(lane48 > half, 1.0, 0.0).astype(F32)
    m5 = jnp.where(lane48 == half, -0.5, m3).astype(F32)
    scale = 1.0 / math.sqrt(total * width)

    def outer_wait(k):
        arrived(recv2[k], CHUNKS + k)

    def outer_stage(k):
        size = SIZES[k]
        held = work.at[pl.ds(0, n * size)]
        held[...] = flat(recv2[k])
        parts = [held[pl.ds(i, n, stride=size), :] for i in range(size)]
        for i in range(size):
            ea, eb, lhs = parts[i], parts[size - 1 - i], tab
            if k == 0 and i in (0, size - 1):
                eb = jnp.where(at_zero, ea, eb)
            if k == 0 and i == 0:
                lhs = tab_zero
            ra = pltpu.roll(ea, half, 1)
            rb = pltpu.roll(eb, half, 1)
            z = jnp.concatenate(
                [
                    (ea * m1).astype(BF16),
                    (ra * m2).astype(BF16),
                    (eb * m3 + rb * m4).astype(BF16),
                    (eb * m4 + rb * m5).astype(BF16),
                ],
                axis=0,
            )
            held[pl.ds(i, n, stride=size), :] = dot(lhs, z) * scale
        send3[k][...] = blocks(held[...])
        post(send3[k], recv3[k], CHUNKS + parts_ + k)


    def ring(ca, slot, h, peer, s_sem, r_sem):
        piece_rows = n * SIZES[ca] // 2
        at = gath[ca].at[slot].at[pl.ds(h * piece_rows, piece_rows)]
        return pltpu.make_async_remote_copy(
            src_ref=at,
            dst_ref=at,
            send_sem=s_sem,
            recv_sem=r_sem,
            device_id={"col": peer},
            device_id_type=MESH,
        )

    def go(*args):
        ring(*args).start()

    def gather_start(ca):
        with jax.named_scope(f"wait3_{ca}"):
            arrived(recv3[ca], CHUNKS + parts_ + ca)
        gath[ca][col] = dot(orders[SIZES[ca]], flat(recv3[ca]).astype(BF16)).astype(BF16)
        go(ca, col, 0, right, ss_sem.at[ca], rr_sem.at[ca, 0])
        go(ca, col, 1, left, ss_sem.at[ca], lr_sem.at[ca, 0])
        go(ca, col, 1, right, ss_sem.at[ca], rr_sem.at[ca, 1])
        go(ca, col, 0, left, ss_sem.at[ca], lr_sem.at[ca, 1])
        go(ca, col, 0, sib, ss_sem.at[ca], sr_sem.at[ca])
        go(ca, col, 1, sib, ss_sem.at[ca], sr_sem.at[ca])

    steps = ncol // 2 - 1

    def gather_step(ca, i):
        dist = i // 2 + 1
        slot = lax.rem(col + ncol - 2 * dist, ncol)
        h = i % 2
        ring(ca, slot, h, right, ss_sem.at[ca], rr_sem.at[ca, i]).wait_recv()
        if i + 2 < steps:
            go(ca, slot, h, right, ss_sem.at[ca], rr_sem.at[ca, i + 2])
        go(ca, slot, h, sib, ss_sem.at[ca], sr_sem.at[ca])
        slot = lax.rem(col + 2 * dist, ncol)
        h = 1 - i % 2
        ring(ca, slot, h, left, ss_sem.at[ca], lr_sem.at[ca, i]).wait_recv()
        if i + 2 < steps:
            go(ca, slot, h, left, ss_sem.at[ca], lr_sem.at[ca, i + 2])
        go(ca, slot, h, sib, ss_sem.at[ca], sr_sem.at[ca])

    def project(ca):
        whole = gath[ca].at[pl.ds(0, ncol // 2)]
        pltpu.make_async_copy(whole, whole, sr_sem.at[ca]).wait()
        acc = None
        for y in range(ncol // 2):
            lhs = jnp.concatenate([gath[ca][2 * y], gath[ca][2 * y + 1]], axis=1)
            term = dot(lhs, wout[pl.ds(2 * width * y, 2 * width), :])
            acc = term if acc is None else acc + term
        low = n * SIZES[ca] // 2
        first = n * starts[ca] // 2
        out[pl.ds(first, low), :] = acc[:low].astype(BF16)
        upper[pl.ds(rows // 2 - first - low, low), :] = acc[low:]

    def steps_of(ca, first, last):
        for i in range(first, last):
            gather_step(ca, i)

    sent = [recv1.at[0]] * CHUNKS + list(recv2) + list(recv3)

    def drain(ca):
        whole = gath[ca].at[pl.ds(0, 2 * steps + 1)]
        pltpu.make_async_copy(whole, whole, ss_sem.at[ca]).wait()

    def drain_exchanges():
        for which, ref in enumerate(sent):
            whole = ref.at[pl.ds(0, n - 1)]
            pltpu.make_async_copy(whole, whole, xs.at[which]).wait()

    with jax.named_scope("W0"):
        outer_wait(0)
    with jax.named_scope("O0"):
        outer_stage(0)
    with jax.named_scope("P2"):
        post2(2)
    with jax.named_scope("W1"):
        outer_wait(1)
    with jax.named_scope("O1"):
        outer_stage(1)
    with jax.named_scope("G0"):
        gather_start(0)
    with jax.named_scope("W2"):
        outer_wait(2)
    with jax.named_scope("O2"):
        outer_stage(2)
    with jax.named_scope("S00"):
        gather_step(0, 0)
    with jax.named_scope("S01"):
        gather_step(0, 1)
    with jax.named_scope("G1"):
        gather_start(1)
    with jax.named_scope("S02"):
        gather_step(0, 2)
    with jax.named_scope("S03"):
        gather_step(0, 3)
    with jax.named_scope("S10"):
        gather_step(1, 0)
    with jax.named_scope("S11"):
        gather_step(1, 1)
    with jax.named_scope("S04"):
        gather_step(0, 4)
    with jax.named_scope("S05"):
        gather_step(0, 5)
    with jax.named_scope("G2"):
        gather_start(2)
    with jax.named_scope("S12"):
        gather_step(1, 2)
    with jax.named_scope("S13"):
        gather_step(1, 3)
    with jax.named_scope("S06"):
        gather_step(0, 6)
    with jax.named_scope("S20"):
        gather_step(2, 0)
    with jax.named_scope("S21"):
        gather_step(2, 1)
    with jax.named_scope("S14"):
        gather_step(1, 4)
    with jax.named_scope("S15"):
        gather_step(1, 5)
    with jax.named_scope("S22"):
        gather_step(2, 2)
    with jax.named_scope("S23"):
        gather_step(2, 3)
    with jax.named_scope("S16"):
        gather_step(1, 6)
    with jax.named_scope("J0"):
        project(0)
    with jax.named_scope("S24"):
        gather_step(2, 4)
    with jax.named_scope("S25"):
        gather_step(2, 5)
    with jax.named_scope("D"):
        for ca in range(parts_ - 1):
            drain(ca)
        drain_exchanges()
    with jax.named_scope("S26"):
        gather_step(2, 6)
    with jax.named_scope("J1"):
        project(1)
    with jax.named_scope("J2"):
        project(2)
    with jax.named_scope("finish"):
        edge = [upper[pl.ds(n * k, 1), :] for k in range(n // 4)]
        for k in range(n // 4):
            upper[pl.ds(n * ((k + 1) % (n // 4)), 1), :] = edge[k]
        out[pl.ds(rows // 2, rows // 2), :] = upper[...].astype(BF16)
    drain(parts_ - 1)


def on_device(tokens, proj_in, proj_out):
    n = lax.axis_size("row")
    ncol = lax.axis_size("col")
    rows, depth = tokens.shape
    width = proj_in.shape[1]
    part = rows // CHUNKS
    steps = ncol // 2 - 1
    count = len(SIZES)
    anywhere = pl.BlockSpec(memory_space=pltpu.HBM)
    message = pltpu.VMEM((CHUNKS, n, part // n, width), BF16)
    dma = pltpu.SemaphoreType.DMA
    return pl.pallas_call(
        functools.partial(kernel, n, ncol),
        out_shape=pltpu.VMEM((rows, proj_out.shape[1]), BF16),
        in_specs=[anywhere] * 3,
        out_specs=pl.BlockSpec(memory_space=pltpu.VMEM),
        scratch_shapes=[
            pltpu.VMEM(tokens.shape, BF16),
            pltpu.VMEM(proj_in.shape, BF16),
            pltpu.VMEM(proj_out.shape, BF16),
            pltpu.VMEM((2 * rows, rows), BF16),
            pltpu.VMEM((n, rows), F32),
            pltpu.VMEM((n, rows), F32),
            pltpu.VMEM((part, width), F32),
            pltpu.VMEM((2 * rows, width), F32),
            message,
            message,
            pltpu.VMEM((rows // 2, proj_out.shape[1]), F32),
            dma((CHUNKS + 2,)),
            dma((CHUNKS + 2 * count,)),
            dma((CHUNKS + 2 * count,)),
            dma((count, steps)),
            dma((count, steps)),
            dma((count,)),
            dma((count,)),
            *(pltpu.VMEM((n, size, width), BF16) for _ in range(4) for size in SIZES),
            *(pltpu.VMEM((ncol, n * size, width), BF16) for size in SIZES),
        ],
        compiler_params=pltpu.CompilerParams(
            collective_id=0, has_side_effects=True, vmem_limit_bytes=66000000
        ),
    )(tokens, proj_in, proj_out)


def solution(mesh):
    return jax.shard_map(
        on_device,
        mesh=mesh,
        in_specs=(P("row", None), P(None, "col"), P(None, "col")),
        out_specs=P("row", "col"),
        check_vma=False,
    )
```

```python
import functools
import math

import jax
import jax.numpy as jnp
from jax import lax
from jax.experimental import pallas as pl
from jax.experimental.pallas import tpu as pltpu
from jax.sharding import PartitionSpec as P

MESH = pl.DeviceIdType.MESH
BF16 = jnp.bfloat16
F32 = jnp.float32
CHUNKS = 3
SIZES = (8, 8, 8)


def turn(phase, period):
    wraps = jnp.floor(phase * (1.0 / period) + 0.5)
    x = (phase - wraps * period) * (math.pi / period)
    y = x * x
    s = 1.0 + y * (-1 / 6 + y * (1 / 120 + y * (-1 / 5040 + y * (1 / 362880 + y * (-1 / 39916800)))))
    c = 1.0 + y * (
        -1 / 2 + y * (1 / 24 + y * (-1 / 720 + y * (1 / 40320 + y * (-1 / 3628800 + y * (1 / 479001600)))))
    )
    s = s * x
    return 1.0 - 2.0 * s * s, 2.0 * s * c


def iota(shape, axis):
    return lax.broadcasted_iota(jnp.int32, shape, axis)


def dot(a, b):
    return jnp.dot(a, b, preferred_element_type=F32)


def kernel(
    n,
    ncol,
    tokens,
    proj_in,
    proj_out,
    out,
    tok,
    win,
    wout,
    table,
    base_c,
    base_s,
    work,
    gacc,
    send1,
    recv1,
    upper,
    load_sem,
    xs,
    xr,
    rr_sem,
    lr_sem,
    ss_sem,
    sr_sem,
    *rest,
):
    parts_ = len(SIZES)
    send2, recv2, send3, recv3, gath = (rest[k * parts_ : (k + 1) * parts_] for k in range(5))
    starts = [sum(SIZES[:c]) for c in range(parts_)]
    rank = lax.axis_index("row")
    col = lax.axis_index("col")
    core = lax.rem(col, 2)
    right = lax.rem(col + 2, ncol)
    left = lax.rem(col + ncol - 2, ncol)
    sib = col + 1 - 2 * core
    rows, depth = tokens.shape
    width = proj_in.shape[1]
    half = width // 2
    total = rows * n
    part = rows // CHUNKS
    per = part // n

    barrier = pltpu.get_barrier_semaphore()

    def greet(s, carry):
        pl.semaphore_signal(
            barrier, inc=1, device_id={"row": lax.rem(rank + s, n)}, device_id_type=MESH
        )
        return carry

    lax.fori_loop(1, n, greet, 0)
    for peer in (right, left, sib):
        pl.semaphore_signal(barrier, inc=1, device_id={"col": peer}, device_id_type=MESH)

    load_in = pltpu.make_async_copy(proj_in, win, load_sem.at[CHUNKS])
    load_in.start()
    loads = []
    for c in range(CHUNKS):
        block = pl.ds(c * part, part)
        load = pltpu.make_async_copy(tokens.at[block], tok.at[block], load_sem.at[c])
        load.start()
        loads.append(load)
    load_out = pltpu.make_async_copy(proj_out, wout, load_sem.at[CHUNKS + 1])
    load_out.start()

    def post(src, dst, which):
        def send(peer):
            pltpu.make_async_remote_copy(
                src_ref=src.at[peer],
                dst_ref=dst.at[rank],
                send_sem=xs.at[which],
                recv_sem=xr.at[which],
                device_id={"row": peer},
                device_id_type=MESH,
            ).start()

        def both(s, carry):
            up = rank + (n // 2 - s)
            down = rank - (n // 2 - s)
            send(jnp.where(up >= n, up - n, up))
            send(jnp.where(down < 0, down + n, down))
            return carry

        opposite = rank + n // 2
        send(jnp.where(opposite >= n, opposite - n, opposite))
        lax.fori_loop(1, n // 2, both, 0)
        dst[rank] = src[rank]

    def post2(k):
        post(send2[k], recv2[k], CHUNKS + k)

    def arrived(dst, which):
        rest = dst.at[pl.ds(0, n - 1)]
        pltpu.make_async_copy(rest, rest, xr.at[which]).wait()

    def flat(ref):
        return ref[...].astype(F32).reshape(n * ref.shape[1], width)

    def blocks(value):
        return value.reshape(n, value.shape[0] // n, width).astype(BF16)

    lane = iota((width, width), 1)
    j = iota((width, width), 0)
    l = jnp.where(lane < half, lane, jnp.where(lane == half, half, lane - half))
    cc, sc = turn((j * l).astype(F32), width)
    chan = jnp.where(lane <= half, cc, -sc).astype(BF16)

    load_in.wait()
    for c in range(CHUNKS):
        with jax.named_scope(f"tokens{c}"):
            loads[c].wait()
        with jax.named_scope(f"branch{c}"):
            x = dot(tok[pl.ds(c * part, part), :], win[...]).astype(BF16)
            work[...] = dot(x, chan)
            for p in range(n):
                send1[c, p] = work[pl.ds(p, per, stride=n), :].astype(BF16)
        if c == 0:
            with jax.named_scope("barrier"):
                pl.semaphore_wait(barrier, n - 1 + 3)
        with jax.named_scope(f"post1_{c}"):
            post(send1.at[c], recv1.at[c], c)

    with jax.named_scope("tables"):
        lanes = rows
        li = iota((8, lanes), 1)
        cq = jnp.where(li >= 2 * part, 2, jnp.where(li >= part, 1, 0))
        rem = li - cq * part
        t = n // 2 * (rem // per) + per * cq + rem % per
        time = (n * t + rank).astype(F32)
        ri = iota((8, lanes), 0)
        for g in range(n // 8):
            bc, bs = turn((ri + 8 * g).astype(F32) * time, total)
            base_c[pl.ds(8 * g, 8), :] = bc
            base_s[pl.ds(8 * g, 8), :] = bs

        for c, size in enumerate(SIZES):
            start = starts[c] // 2
            place = ri % size
            lower = place < size // 2
            num = jnp.where(lower, start + place, 25 - start - size + place)
            sigma = jnp.where(lower, 1.0, -1.0).astype(F32)
            wc, ws = turn(num.astype(F32) * time, rows)
            wcs, wss = wc * sigma, ws * sigma
            each = 8 // size
            row = 2 * n * starts[c]

            def unit(u, wc=wc, ws=ws, wcs=wcs, wss=wss, each=each):
                bc = base_c[pl.ds(u * each, 1), :]
                bs = base_s[pl.ds(u * each, 1), :]
                if each == 2:
                    bc = jnp.where(ri < 4, bc, base_c[pl.ds(2 * u + 1, 1), :])
                    bs = jnp.where(ri < 4, bs, base_s[pl.ds(2 * u + 1, 1), :])
                return wc * bc - wss * bs, ws * bc + wcs * bs

            def put(pair, first, second, row=row, size=size):
                at = pl.multiple_of(row + 16 * pair, 16)
                table[pl.ds(at, 16), :] = jnp.concatenate([first[0], second[0]], axis=0).astype(BF16)
                at = pl.multiple_of(row + n * size + 16 * pair, 16)
                table[pl.ds(at, 16), :] = jnp.concatenate([first[1], second[1]], axis=0).astype(BF16)

            def body(pair, carry, unit=unit, put=put):
                put(pair, unit(2 * pair), unit(2 * pair + 1))
                return carry

            lax.fori_loop(0, n * size // 16, body, 0)
            if c == 0:
                mc, ms = turn(jnp.float32(12.0) * time, rows)
                oc, os = unit(0)
                mid = ri == size - 1
                put(0, (jnp.where(mid, mc, oc), jnp.where(mid, ms, os)), unit(1))

    with jax.named_scope("tables2"):
        bi = iota((n, 4 * n), 0)
        pi = iota((n, 4 * n), 1)
        quarter = jnp.where(pi >= 3 * n, 3, jnp.where(pi >= 2 * n, 2, jnp.where(pi >= n, 1, 0)))
        pp = pi - quarter * n

        def outer(flip):
            bb = jnp.where(quarter < 2, bi, flip - bi)
            oc, os = turn((bb * pp).astype(F32), n)
            return jnp.where((quarter == 0) | (quarter == 2), oc, os)

        at_zero = rank == 0
        tab = outer(n - 1)
        tab_zero = jnp.where(at_zero, outer(n), tab).astype(BF16)
        tab = tab.astype(BF16)

        qr = iota((width, width), 0)
        qc = iota((width, width), 1)
        chosen = jnp.where(qr <= half, qr, width + half - qr)
        swap = jnp.where(qc == chosen, 1.0, 0.0).astype(BF16)
        load_out.wait()

        def reorder(g, carry):
            at = pl.ds(pl.multiple_of(g * width, width), width)
            wout[at, :] = dot(swap, wout[at, :]).astype(BF16)
            return carry

        lax.fori_loop(0, ncol, reorder, 0)

        orders = {}
        for size in sorted(set(SIZES)):
            pr = iota((n * size, n * size), 0)
            pc = iota((n * size, n * size), 1)
            want_i = pr // n
            want_e = pr - want_i * n
            want_d = jnp.where(want_i < size // 2, want_e, jnp.where(want_e == 0, 0, n - want_e))
            orders[size] = jnp.where(pc == want_d * size + want_i, 1.0, 0.0).astype(BF16)

    sign = jnp.where(iota((part, width), 1) < half, 1.0, -1.0).astype(F32)
    for c in range(CHUNKS):
        with jax.named_scope(f"wait1_{c}"):
            arrived(recv1.at[c], c)
        data = flat(recv1.at[c]).astype(BF16)
        for k, size in enumerate(SIZES):
            at = pl.ds(2 * n * starts[k], 2 * n * size)
            got = dot(table[at, pl.ds(c * part, part)], data)
            if c > 0:
                got = gacc[at, :] + got
            if c < CHUNKS - 1:
                gacc[at, :] = got
            else:
                value = got[: n * size] + pltpu.roll(got[n * size :], half, 1) * sign[: n * size]
                send2[k][...] = blocks(value)
                if k < 2:
                    with jax.named_scope(f"post2_{k}"):
                        post2(k)

    lane48 = iota((n, width), 1)
    m1 = jnp.where((lane48 == 0) | (lane48 == half), 0.5, jnp.where(lane48 < half, 1.0, 0.0)).astype(F32)
    m2 = jnp.where(lane48 == half, -0.5, m1).astype(F32)
    m3 = jnp.where((lane48 == 0) | (lane48 == half), 0.5, 0.0).astype(F32)
    m4 = jnp.where(lane48 > half, 1.0, 0.0).astype(F32)
    m5 = jnp.where(lane48 == half, -0.5, m3).astype(F32)
    scale = 1.0 / math.sqrt(total * width)

    def outer_wait(k):
        arrived(recv2[k], CHUNKS + k)

    def outer_stage(k):
        size = SIZES[k]
        held = work.at[pl.ds(0, n * size)]
        held[...] = flat(recv2[k])
        parts = [held[pl.ds(i, n, stride=size), :] for i in range(size)]
        for i in range(size):
            ea, eb, lhs = parts[i], parts[size - 1 - i], tab
            if k == 0 and i in (0, size - 1):
                eb = jnp.where(at_zero, ea, eb)
            if k == 0 and i == 0:
                lhs = tab_zero
            ra = pltpu.roll(ea, half, 1)
            rb = pltpu.roll(eb, half, 1)
            z = jnp.concatenate(
                [
                    (ea * m1).astype(BF16),
                    (ra * m2).astype(BF16),
                    (eb * m3 + rb * m4).astype(BF16),
                    (eb * m4 + rb * m5).astype(BF16),
                ],
                axis=0,
            )
            held[pl.ds(i, n, stride=size), :] = dot(lhs, z) * scale
        send3[k][...] = blocks(held[...])
        post(send3[k], recv3[k], CHUNKS + parts_ + k)


    def ring(ca, slot, h, peer, s_sem, r_sem):
        piece_rows = n * SIZES[ca] // 2
        at = gath[ca].at[slot].at[pl.ds(h * piece_rows, piece_rows)]
        return pltpu.make_async_remote_copy(
            src_ref=at,
            dst_ref=at,
            send_sem=s_sem,
            recv_sem=r_sem,
            device_id={"col": peer},
            device_id_type=MESH,
        )

    def go(*args):
        ring(*args).start()

    def gather_start(ca):
        with jax.named_scope(f"wait3_{ca}"):
            arrived(recv3[ca], CHUNKS + parts_ + ca)
        gath[ca][col] = dot(orders[SIZES[ca]], flat(recv3[ca]).astype(BF16)).astype(BF16)
        go(ca, col, 0, right, ss_sem.at[ca], rr_sem.at[ca, 0])
        go(ca, col, 1, left, ss_sem.at[ca], lr_sem.at[ca, 0])
        go(ca, col, 1, right, ss_sem.at[ca], rr_sem.at[ca, 1])
        go(ca, col, 0, left, ss_sem.at[ca], lr_sem.at[ca, 1])
        go(ca, col, 0, sib, ss_sem.at[ca], sr_sem.at[ca, 0])
        go(ca, col, 1, sib, ss_sem.at[ca], sr_sem.at[ca, 0])

    steps = ncol // 2 - 1

    def gather_step(ca, i):
        dist = i // 2 + 1
        slot = lax.rem(col + ncol - 2 * dist, ncol)
        h = i % 2
        ring(ca, slot, h, right, ss_sem.at[ca], rr_sem.at[ca, i]).wait_recv()
        if i + 2 < steps:
            go(ca, slot, h, right, ss_sem.at[ca], rr_sem.at[ca, i + 2])
        go(ca, slot, h, sib, ss_sem.at[ca], sr_sem.at[ca, i // (steps - 1)])
        slot = lax.rem(col + 2 * dist, ncol)
        h = 1 - i % 2
        ring(ca, slot, h, left, ss_sem.at[ca], lr_sem.at[ca, i]).wait_recv()
        if i + 2 < steps:
            go(ca, slot, h, left, ss_sem.at[ca], lr_sem.at[ca, i + 2])
        go(ca, slot, h, sib, ss_sem.at[ca], sr_sem.at[ca, i // (steps - 1)])

    def project(ca):
        acc = None
        for k in range(ncol // 2):
            if k == 0:
                whole = gath[ca].at[pl.ds(0, ncol // 2 - 1)]
                pltpu.make_async_copy(whole, whole, sr_sem.at[ca, 0]).wait()
            if k == ncol // 2 - 1:
                whole = gath[ca].at[pl.ds(0, 1)]
                pltpu.make_async_copy(whole, whole, sr_sem.at[ca, 1]).wait()
            y = lax.rem(col // 2 + (ncol // 4 + 1) + k, ncol // 2)
            lhs = jnp.concatenate([gath[ca][2 * y], gath[ca][2 * y + 1]], axis=1)
            at = pl.ds(pl.multiple_of(2 * width * y, 2 * width), 2 * width)
            term = dot(lhs, wout[at, :])
            acc = term if acc is None else acc + term
        low = n * SIZES[ca] // 2
        first = n * starts[ca] // 2
        out[pl.ds(first, low), :] = acc[:low].astype(BF16)
        upper[pl.ds(rows // 2 - first - low, low), :] = acc[low:]

    def steps_of(ca, first, last):
        for i in range(first, last):
            gather_step(ca, i)

    sent = [recv1.at[0]] * CHUNKS + list(recv2) + list(recv3)

    def drain(ca):
        whole = gath[ca].at[pl.ds(0, 2 * steps + 1)]
        pltpu.make_async_copy(whole, whole, ss_sem.at[ca]).wait()

    def drain_exchanges():
        for which, ref in enumerate(sent):
            whole = ref.at[pl.ds(0, n - 1)]
            pltpu.make_async_copy(whole, whole, xs.at[which]).wait()

    with jax.named_scope("W0"):
        outer_wait(0)
    with jax.named_scope("O0"):
        outer_stage(0)
    with jax.named_scope("P2"):
        post2(2)
    with jax.named_scope("W1"):
        outer_wait(1)
    with jax.named_scope("O1"):
        outer_stage(1)
    with jax.named_scope("G0"):
        gather_start(0)
    with jax.named_scope("W2"):
        outer_wait(2)
    with jax.named_scope("O2"):
        outer_stage(2)
    with jax.named_scope("S00"):
        gather_step(0, 0)
    with jax.named_scope("S01"):
        gather_step(0, 1)
    with jax.named_scope("G1"):
        gather_start(1)
    with jax.named_scope("S02"):
        gather_step(0, 2)
    with jax.named_scope("S03"):
        gather_step(0, 3)
    with jax.named_scope("S10"):
        gather_step(1, 0)
    with jax.named_scope("S11"):
        gather_step(1, 1)
    with jax.named_scope("S04"):
        gather_step(0, 4)
    with jax.named_scope("S05"):
        gather_step(0, 5)
    with jax.named_scope("G2"):
        gather_start(2)
    with jax.named_scope("S12"):
        gather_step(1, 2)
    with jax.named_scope("S13"):
        gather_step(1, 3)
    with jax.named_scope("S06"):
        gather_step(0, 6)
    with jax.named_scope("S20"):
        gather_step(2, 0)
    with jax.named_scope("S21"):
        gather_step(2, 1)
    with jax.named_scope("S14"):
        gather_step(1, 4)
    with jax.named_scope("S15"):
        gather_step(1, 5)
    with jax.named_scope("S22"):
        gather_step(2, 2)
    with jax.named_scope("S23"):
        gather_step(2, 3)
    with jax.named_scope("S16"):
        gather_step(1, 6)
    with jax.named_scope("J0"):
        project(0)
    with jax.named_scope("S24"):
        gather_step(2, 4)
    with jax.named_scope("S25"):
        gather_step(2, 5)
    with jax.named_scope("D"):
        for ca in range(parts_ - 1):
            drain(ca)
        drain_exchanges()
    with jax.named_scope("S26"):
        gather_step(2, 6)
    with jax.named_scope("J1"):
        project(1)
    with jax.named_scope("J2"):
        project(2)
    with jax.named_scope("finish"):
        edge = [upper[pl.ds(n * k, 1), :] for k in range(n // 4)]
        for k in range(n // 4):
            upper[pl.ds(n * ((k + 1) % (n // 4)), 1), :] = edge[k]
        out[pl.ds(rows // 2, rows // 2), :] = upper[...].astype(BF16)
    drain(parts_ - 1)


def on_device(tokens, proj_in, proj_out):
    n = lax.axis_size("row")
    ncol = lax.axis_size("col")
    rows, depth = tokens.shape
    width = proj_in.shape[1]
    part = rows // CHUNKS
    steps = ncol // 2 - 1
    count = len(SIZES)
    anywhere = pl.BlockSpec(memory_space=pltpu.HBM)
    message = pltpu.VMEM((CHUNKS, n, part // n, width), BF16)
    dma = pltpu.SemaphoreType.DMA
    return pl.pallas_call(
        functools.partial(kernel, n, ncol),
        out_shape=pltpu.VMEM((rows, proj_out.shape[1]), BF16),
        in_specs=[anywhere] * 3,
        out_specs=pl.BlockSpec(memory_space=pltpu.VMEM),
        scratch_shapes=[
            pltpu.VMEM(tokens.shape, BF16),
            pltpu.VMEM(proj_in.shape, BF16),
            pltpu.VMEM(proj_out.shape, BF16),
            pltpu.VMEM((2 * rows, rows), BF16),
            pltpu.VMEM((n, rows), F32),
            pltpu.VMEM((n, rows), F32),
            pltpu.VMEM((part, width), F32),
            pltpu.VMEM((2 * rows, width), F32),
            message,
            message,
            pltpu.VMEM((rows // 2, proj_out.shape[1]), F32),
            dma((CHUNKS + 2,)),
            dma((CHUNKS + 2 * count,)),
            dma((CHUNKS + 2 * count,)),
            dma((count, steps)),
            dma((count, steps)),
            dma((count,)),
            dma((count, 2)),
            *(pltpu.VMEM((n, size, width), BF16) for _ in range(4) for size in SIZES),
            *(pltpu.VMEM((ncol, n * size, width), BF16) for size in SIZES),
        ],
        compiler_params=pltpu.CompilerParams(
            collective_id=0, has_side_effects=True, vmem_limit_bytes=66000000
        ),
    )(tokens, proj_in, proj_out)


def solution(mesh):
    return jax.shard_map(
        on_device,
        mesh=mesh,
        in_specs=(P("row", None), P(None, "col"), P(None, "col")),
        out_specs=P("row", "col"),
        check_vma=False,
    )
```
